768 devices in a mesh: fs: 24 (over z, core), tp: 32 (over y, x).
Axes of the slice: x: 4, y: 8, z: 12, core: 2. Of those that a mesh axis runs over, the one named last changes fastest.
Arguments:
- block_in: bfloat16 [24576, 2304], P('fs'), may hold values from -6 to 6
- out_cot: bfloat16 [24576, 2304], P('fs'), may hold values from -6 to 6
- gated_out: bfloat16 [24576, 4608], P('fs', 'tp'), may hold values from -6 to 6
- gate_cot: bfloat16 [24576, 4608], P('fs', 'tp'), may hold values from -6 to 6
- factor_out: bfloat16 [2304, 192], P('fs'), may hold values from -0.104166667 to 0.104166667
- factor_z: bfloat16 [2304, 192], P('fs'), may hold values from -0.104166667 to 0.104166667
- weight_out: float32 [4608, 2304], P('tp', 'fs'), may hold values from -0.09375 to 0.09375
- weight_z: float32 [2304, 4608], P('fs', 'tp'), may hold values from -0.125 to 0.125
- first_out: float32 [4608, 192], P('tp', 'fs'), may hold values from -1254.13875 to 1254.13875
- second_out: float32 [4608, 192], P('tp', 'fs'), may hold values from 4915.2 to 122880
- first_z: float32 [192, 4608], P('fs', 'tp'), may hold values from -1254.13875 to 1254.13875
- second_z: float32 [192, 4608], P('fs', 'tp'), may hold values from 4915.2 to 122880
Outputs:
- step_out: float32 [4608, 2304], P('tp', 'fs')
- step_z: float32 [2304, 4608], P('fs', 'tp')
- new_first_out: float32 [4608, 192], P('tp', 'fs')
- new_second_out: float32 [4608, 192], P('tp', 'fs')
- new_first_z: float32 [192, 4608], P('fs', 'tp')
- new_second_z: float32 [192, 4608], P('fs', 'tp')
- copy_out: bfloat16 [4608, 2304], P('tp')
- copy_z: bfloat16 [2304, 4608], P(None, 'tp')
The draws below stay inside these ranges and needn't reach their ends.
All inputs are finite; a program needn't handle non-finite values.
Results may differ from the reference program's by a relative error of at most 0.0018.
Values may be sent and summed in bfloat16 or wider, within the bound.
No kernel may reach another device: no remote copies, remote signals or barrier semaphores. Data moves between devices by JAX's collectives and lax.ppermute only.
A program may use at most 32 MiB of HBM per device.

```python
import math
import jax
import jax.numpy as jnp
from jax import lax

D = 2304
INNER = 4608
RANK = 192
TOKENS = 24576


def shared_parts(key, member):
    folded = jax.random.fold_in(key, 1000 + member)
    subkeys = jax.random.split(folded, 4)
    width_dir = jnp.clip(jax.random.normal(subkeys[0], (D,), jnp.float32), -3.0, 3.0)
    inner_dir = jnp.clip(jax.random.normal(subkeys[1], (INNER,), jnp.float32), -3.0, 3.0)
    rank_wts = jax.random.uniform(subkeys[2], (RANK,), jnp.float32, 0.5, 1.5)
    token_sign = (2 * jax.random.randint(subkeys[3], (TOKENS,), 0, 2) - 1).astype(jnp.float32)
    return (width_dir, inner_dir, rank_wts, token_sign)


def noise_field(key, label_code, array_shape, clip_bound):
    subkey = jax.random.fold_in(key, label_code)
    return jnp.clip(jax.random.normal(subkey, array_shape, jnp.float32), -clip_bound, clip_bound)


def coupling_level():
    return min(math.sqrt(15.0 / math.sqrt(D * TOKENS)), 0.5)


def token_field(key, member, label_code, use_width):
    width_dir, inner_dir, rank_wts, token_sign = shared_parts(key, member)
    if use_width:
        common_dir = width_dir
        columns = D
    else:
        common_dir = inner_dir
        columns = INNER
    drawn = noise_field(key, label_code, (TOKENS, columns), 4.0)
    drawn = drawn + coupling_level() * token_sign[:, None] * common_dir[None, :]
    return jnp.clip(drawn, -6.0, 6.0).astype(jnp.bfloat16)


def factor_field(key, member, label_code):
    width_dir, inner_dir, rank_wts, token_sign = shared_parts(key, member)
    spread = D ** (-0.5)
    drawn = spread * noise_field(key, label_code, (D, RANK), 4.0)
    drawn = drawn + 0.1 * spread * width_dir[:, None] * rank_wts[None, :]
    return jnp.clip(drawn, -5.0 * spread, 5.0 * spread).astype(jnp.bfloat16)


def draw_block_in(key, part):
    return token_field(key, 2, 11, True)


def draw_gate_cot(key, part):
    return token_field(key, 2, 12, False)


def draw_out_cot(key, part):
    return token_field(key, 1, 13, True)


def draw_gated_out(key, part):
    return token_field(key, 1, 14, False)


def draw_factor_out(key, part):
    return factor_field(key, 1, 15)


def draw_factor_z(key, part):
    return factor_field(key, 2, 16)


def draw_first_out(key, part):
    width_dir, inner_dir, rank_wts, token_sign = shared_parts(key, 1)
    root_tokens = math.sqrt(TOKENS)
    drawn = noise_field(key, 17, (INNER, RANK), 4.0) + 0.8 * inner_dir[:, None] * rank_wts[None, :]
    return jnp.clip(root_tokens * drawn, -8.0 * root_tokens, 8.0 * root_tokens)


def draw_first_z(key, part):
    width_dir, inner_dir, rank_wts, token_sign = shared_parts(key, 2)
    root_tokens = math.sqrt(TOKENS)
    drawn = noise_field(key, 18, (RANK, INNER), 4.0) + 0.8 * rank_wts[:, None] * inner_dir[None, :]
    return jnp.clip(root_tokens * drawn, -8.0 * root_tokens, 8.0 * root_tokens)


def level_of(own_key, extent, pieces, low, high):
    loudness, own = 1.0, jax.random.fold_in(own_key, 6)
    for position, blocks in pieces:
        draws = jnp.exp(jax.random.uniform(jax.random.fold_in(own, position), (blocks,), jnp.float32, low / len(pieces), high / len(pieces)))
        loudness = loudness * jnp.repeat(draws, extent[position] // blocks).reshape([-1 if axis == position else 1 for axis in range(len(extent))])
    return loudness


def scatter_about(own_key, dims, scale, reach, cuts=(), kind=jnp.bfloat16):
    result = scale * jax.random.normal(own_key, dims, jnp.float32)
    if cuts:
        result = result * level_of(own_key, dims, cuts, -0.22, 0.18)
    return jnp.clip(result, -reach, reach).astype(kind)


def setup_inputs(seed: int = 0) -> dict:
    key_list = jax.random.split(jax.random.key(seed), 13)
    return {
        "block_in": draw_block_in(jax.random.fold_in(key_list[12], 71), 0),
        "out_cot": draw_out_cot(jax.random.fold_in(key_list[12], 71), 0),
        "gated_out": draw_gated_out(jax.random.fold_in(key_list[12], 71), 0),
        "gate_cot": draw_gate_cot(jax.random.fold_in(key_list[12], 71), 0),
        "factor_out": draw_factor_out(jax.random.fold_in(key_list[12], 71), 0),
        "factor_z": draw_factor_z(jax.random.fold_in(key_list[12], 71), 0),
        "weight_out": scatter_about(key_list[6], (INNER, D), INNER ** -0.5, 0.09375, ((0, 32), (1, 24)), jnp.float32),
        "weight_z": scatter_about(key_list[7], (D, INNER), D ** -0.5, 0.125, ((0, 24), (1, 32)), jnp.float32),
        "first_out": draw_first_out(jax.random.fold_in(key_list[12], 71), 0),
        "second_out": jnp.clip(jnp.exp(math.log(122880.0) - 3.218876 * jax.random.uniform(key_list[9], (INNER, RANK), jnp.float32) ** level_of(key_list[9], (INNER, RANK), ((0, 32), (1, 24)), -0.2, 0.2)), 4915.2, 122880.0),
        "first_z": draw_first_z(jax.random.fold_in(key_list[12], 71), 0),
        "second_z": jnp.clip(jnp.exp(math.log(122880.0) - 3.218876 * jax.random.uniform(key_list[11], (RANK, INNER), jnp.float32) ** level_of(key_list[11], (RANK, INNER), ((0, 24), (1, 32)), -0.2, 0.2)), 4915.2, 122880.0),
    }


beta_first = 0.8
beta_second = 0.9
adam_eps = 1e-08
norm_eps = 1e-06
rate = 0.005

def moments(first, second, gradient):
    new_first = beta_first * first + (1.0 - beta_first) * gradient
    new_second = beta_second * second + (1.0 - beta_second) * gradient * gradient
    return (new_first, new_second, new_first / (jnp.sqrt(new_second) + adam_eps))

def reference(block_in, out_cot, gated_out, gate_cot, factor_out, factor_z, weight_out, weight_z, first_out, second_out, first_z, second_z):
    proj_cot = jnp.dot(out_cot.astype(jnp.float32), factor_out.astype(jnp.float32), precision=lax.Precision.HIGHEST)
    proj_input = jnp.dot(block_in.astype(jnp.float32), factor_z.astype(jnp.float32), precision=lax.Precision.HIGHEST)
    grad_out = jnp.dot(gated_out.astype(jnp.float32).T, proj_cot, precision=lax.Precision.HIGHEST)
    grad_z = jnp.dot(proj_input.T, gate_cot.astype(jnp.float32), precision=lax.Precision.HIGHEST)
    new_first_out, new_second_out, dir_out = moments(first_out, second_out, grad_out)
    new_first_z, new_second_z, dir_z = moments(first_z, second_z, grad_z)
    update_out = jnp.dot(dir_out, factor_out.astype(jnp.float32).T, precision=lax.Precision.HIGHEST)
    update_z = jnp.dot(factor_z.astype(jnp.float32), dir_z, precision=lax.Precision.HIGHEST)
    step_out = update_out * lax.rsqrt(jnp.mean(update_out * update_out) + norm_eps)
    step_z = update_z * lax.rsqrt(jnp.mean(update_z * update_z) + norm_eps)
    copy_out = (weight_out - rate * step_out).astype(jnp.bfloat16)
    copy_z = (weight_z - rate * step_z).astype(jnp.bfloat16)
    return (step_out, step_z, new_first_out, new_second_out, new_first_z, new_second_z, copy_out, copy_z)
```

```python
import jax
import jax.numpy as jnp
from jax import lax
from jax.experimental import pallas as pl
from jax.experimental.pallas import tpu as pltpu
from jax.sharding import Mesh
from jax.sharding import PartitionSpec as P

D = 2304
INNER = 4608
RANK = 192
FS = ("z", "core")
TP = ("y", "x")
RINGS, CORES = 12, 2
PARTS = RINGS * CORES
TPS = 32
CHUNKS = 4
FLYING = 2

beta_first = 0.8
beta_second = 0.9
adam_eps = 1e-08
norm_eps = 1e-06
rate = 0.005

VMEM = pl.BlockSpec(memory_space=pltpu.VMEM)
SMEM = pl.BlockSpec(memory_space=pltpu.SMEM)
HBM = pl.BlockSpec(memory_space=pltpu.HBM)
FLAT = (((1,), (0,)), ((), ()))
TURNED = (((1,), (1,)), ((), ()))


def dot(a, b, dims):
    return lax.dot_general(a, b, dims, preferred_element_type=jnp.float32)


def in_hbm(value):
    return pltpu.with_memory_space_constraint(value, pltpu.HBM)


def in_vmem(value):
    return pltpu.with_memory_space_constraint(value, pltpu.VMEM)


def split_parts(values):
    high_part = values.astype(jnp.bfloat16)
    return high_part, (values - high_part.astype(jnp.float32)).astype(jnp.bfloat16)


def call(kernel, outs, specs, mib, scratch=()):
    return pl.pallas_call(
        kernel,
        out_shape=[
            out[2](out[0], out[1]) if len(out) == 3 else jax.ShapeDtypeStruct(*out) for out in outs
        ],
        in_specs=specs,
        out_specs=[HBM if pltpu.HBM in out else VMEM for out in outs],
        scratch_shapes=scratch,
        compiler_params=pltpu.CompilerParams(vmem_limit_bytes=mib * 1024 * 1024),
    )


def gradient_kernel(
    core, cot, inp, own, other, gated, gate, partial, factor_out, factor_z, kept_out, kept_z,
    tokens, gates, highs, lows, sems, gate_sems, kept_sems,
):
    sides = ((cot, gated, factor_out), (inp, gate, factor_z))
    moves = []
    for k, (source, _, _) in enumerate(sides):
        for c in range(CHUNKS):
            height = tokens.shape[1] // CHUNKS
            at = pl.ds(height * c, height)
            moves.append((k, at, pltpu.make_async_copy(source.at[at], tokens.at[k, at], sems.at[k, c])))
    gate_moves = [
        pltpu.make_async_copy(turned, gates.at[k], gate_sems.at[k]) for k, (_, turned, _) in enumerate(sides)
    ]
    for _, _, move in moves[:FLYING]:
        move.start()

    rows = own.shape[0] // RINGS
    here = core[0] * rows
    there = rows - here
    for z in range(RINGS):
        for shard, place in ((own, here), (other, there)):
            block = shard[rows * z : rows * (z + 1), :]
            at = pl.ds(pl.multiple_of(2 * rows * z + place, 32), rows)
            factor_out[at, :] = block[:, :RANK]
            factor_z[at, :] = block[:, RANK:]

    keeps = [
        pltpu.make_async_copy(factor, kept, kept_sems.at[k])
        for k, (factor, kept) in enumerate(((factor_out, kept_out), (factor_z, kept_z)))
    ]
    width = gated.shape[0]
    for n, (k, at, move) in enumerate(moves):
        move.wait()
        if n + FLYING < len(moves):
            moves[n + FLYING][2].start()
        elif n + FLYING < len(moves) + 2:
            gate_moves[n + FLYING - len(moves)].start()
            keeps[n + FLYING - len(moves)].start()
        high, low = split_parts(dot(tokens[k, at, :], sides[k][2][...], FLAT))
        highs[k, at, :] = high
        lows[k, at, :] = low
    for k, move in enumerate(gate_moves):
        move.wait()
        total = dot(gates[k], highs[k], FLAT) + dot(gates[k], lows[k], FLAT)
        partial[:, k * width : (k + 1) * width] = total.T
    for keep in keeps:
        keep.wait()


def moments_kernel(arrived, first_out, second_out, first_z, second_z, *outs):
    total = jnp.sum(arrived[...], axis=0)
    width = first_out.shape[1]
    ratios = outs[-1]
    for k, (first, second) in enumerate(((first_out, second_out), (first_z, second_z))):
        gradient = total[:, k * width : (k + 1) * width]
        new_first = beta_first * first[...] + (1.0 - beta_first) * gradient
        new_second = beta_second * second[...] + (1.0 - beta_second) * gradient * gradient
        outs[2 * k][...] = new_first
        outs[2 * k + 1][...] = new_second
        ratio = new_first / (jnp.sqrt(new_second) + adam_eps)
        ratios[..., k * width : (k + 1) * width] = jnp.broadcast_to(ratio, ratios.shape[:-1] + (width,))


def turned_parts(ratios, width):
    turned = ratios[...].T
    return [split_parts(turned[k * width : (k + 1) * width]) for k in range(2)]


def sums_kernel(ratios, factor_out, factor_z, sums):
    totals = []
    for (high, low), factor in zip(turned_parts(ratios, ratios.shape[1] // 2), (factor_out, factor_z)):
        update = dot(high, factor[...], TURNED) + dot(low, factor[...], TURNED)
        totals.append(jnp.sum(jnp.sum(update * update, axis=0, keepdims=True), axis=1, keepdims=True))
    lane = lax.broadcasted_iota(jnp.int32, (1, 128), 1)
    row = jnp.where(lane < 64, totals[0], totals[1])
    sums[...] = jnp.broadcast_to(row[None], sums.shape)


def update_kernel(
    place, ratios, kept_out, kept_z, weights, wide, narrow, full, factors, blocks, factor_sems, sem
):
    width, columns = narrow.shape[0] // 2, narrow.shape[1]
    moves = [
        pltpu.make_async_copy(kept, factors.at[k], factor_sems.at[k])
        for k, kept in enumerate((kept_out, kept_z))
    ]
    move = pltpu.make_async_copy(weights, blocks, sem)
    for each in (*moves, move):
        each.start()
    for k, (high, low) in enumerate(turned_parts(ratios, width)):
        rows = pl.ds(k * width, width)
        moves[k].wait()
        wide[rows, :] = dot(high, factors[k], TURNED) + dot(low, factors[k], TURNED)
        mine = factors[k, pl.ds(pl.multiple_of(place[0] * columns, 32), columns), :]
        narrow[rows, :] = dot(high, mine, TURNED) + dot(low, mine, TURNED)
    move.wait()
    for k in range(PARTS):
        full[:, k * columns : (k + 1) * columns] = blocks[k]


def final_kernel(sums, wide, narrow, full, copy_out, copy_z, step_out, step_z):
    width = step_out.shape[0]
    total = jnp.sum(sums[...], axis=0)
    scales = lax.rsqrt(total / (D * INNER) + norm_eps)
    for k, (copy, step) in enumerate(((copy_out, step_out), (copy_z, step_z))):
        scale = scales[:, 64 * k : 64 * k + 1]
        rows = pl.ds(k * width, width)
        step[...] = narrow[rows, :] * scale
        copy[...] = (full[rows, :] - rate * (wide[rows, :] * scale)).astype(jnp.bfloat16)


def per_device(
    block_in, out_cot, gated_out, gate_cot, factor_out, factor_z,
    weight_out, weight_z, first_out, second_out, first_z, second_z,
):
    f32, bf16 = jnp.float32, jnp.bfloat16
    width, columns = weight_out.shape
    ranks = first_z.shape[0]
    tokens = block_in.shape[0]
    core = lax.axis_index("core").reshape(1).astype(jnp.int32)
    place = lax.axis_index(FS).reshape(1).astype(jnp.int32)

    own = lax.all_gather(jnp.concatenate([factor_out, factor_z], axis=1), "z", axis=0, tiled=True)
    if SC_LATE:
        own, weight_out, weight_z = lax.optimization_barrier((own, weight_out, weight_z))
    other = lax.ppermute(own, "core", [(0, 1), (1, 0)])
    weights = jnp.concatenate([weight_out, weight_z.T], axis=0)
    weights = lax.all_gather(weights, FS, axis=0, tiled=True).reshape(PARTS, 2 * width, columns)

    partial, full_out, full_z, kept_out, kept_z = call(
        gradient_kernel,
        [((RANK, 2 * width), f32)] + [((D, RANK), bf16, pltpu.VMEM)] * 2 + [((D, RANK), bf16, pltpu.HBM)] * 2,
        [SMEM, HBM, HBM, VMEM, VMEM, HBM, HBM],
        24,
        [
            pltpu.VMEM((2, tokens, D), bf16),
            pltpu.VMEM((2, width, tokens), bf16),
            pltpu.VMEM((2, tokens, RANK), bf16),
            pltpu.VMEM((2, tokens, RANK), bf16),
            pltpu.SemaphoreType.DMA((2, CHUNKS)),
            pltpu.SemaphoreType.DMA((2,)),
            pltpu.SemaphoreType.DMA((2,)),
        ],
    )(core, in_hbm(out_cot), in_hbm(block_in), in_vmem(own), in_vmem(other), in_hbm(gated_out.T), in_hbm(gate_cot.T))
    arrived = lax.all_to_all(
        partial.reshape(PARTS, ranks, 2 * width), FS, split_axis=0, concat_axis=0, tiled=True
    )
    small = ((ranks, width), f32)
    lead = (PARTS,) if DIR_A2A else ()
    *news, ratios = call(moments_kernel, [small] * 4 + [(lead + (ranks, 2 * width), f32)], [VMEM] * 5, 4)(
        arrived, first_out.T, second_out.T, first_z, second_z
    )
    if DIR_A2A:
        ratios = lax.all_to_all(ratios, FS, split_axis=0, concat_axis=0, tiled=True).reshape(RANK, 2 * width)
    else:
        ratios = lax.all_gather(ratios, FS, axis=0, tiled=True)
    (sums,) = call(sums_kernel, [((TPS, 1, 128), f32)], [VMEM] * 3, 8)(
        ratios, in_vmem(full_out), in_vmem(full_z)
    )
    sums = lax.all_to_all(sums, TP, split_axis=0, concat_axis=0, tiled=True)
    wide, narrow, full = call(
        update_kernel,
        [((2 * width, D), f32, pltpu.VMEM), ((2 * width, columns), f32, pltpu.VMEM), ((2 * width, D), f32, pltpu.VMEM)],
        [SMEM, VMEM, HBM, HBM, HBM],
        16,
        [
            pltpu.VMEM((2, D, RANK), bf16),
            pltpu.VMEM((PARTS, 2 * width, columns), f32),
            pltpu.SemaphoreType.DMA((2,)),
            pltpu.SemaphoreType.DMA,
        ],
    )(place, ratios, in_hbm(kept_out), in_hbm(kept_z), in_hbm(weights))
    copy_out, copy_z, step_out, step_z = call(
        final_kernel,
        [((width, D), bf16), ((width, D), bf16), ((width, columns), f32), ((width, columns), f32)],
        [VMEM] * 4,
        4,
    )(sums, in_vmem(wide), in_vmem(narrow), in_vmem(full))
    return (
        step_out, step_z.T, news[0].T, news[1].T, news[2], news[3], copy_out, copy_z.T,
    )


SC_LATE = True
DIR_A2A = True


def solution(mesh):
    finer = Mesh(mesh.devices.reshape(RINGS, CORES, 8, 4), FS + TP)
    rows, both, turned = P(FS, None), P(FS, TP), P(TP, FS)
    return jax.shard_map(
        per_device,
        mesh=finer,
        in_specs=(
            rows, rows, both, both, rows, rows, turned, both, turned, turned, both, both,
        ),
        out_specs=(turned, both, turned, turned, both, both, P(TP, None), P(None, TP)),
        check_vma=False,
    )
```

```python
import jax
import jax.numpy as jnp
from jax import lax
from jax.experimental import pallas as pl
from jax.experimental.pallas import tpu as pltpu
from jax.sharding import Mesh
from jax.sharding import PartitionSpec as P

D = 2304
INNER = 4608
RANK = 192
FS = ("z", "core")
TP = ("y", "x")
RINGS, CORES = 12, 2
PARTS = RINGS * CORES
TPS = 32
CHUNKS = 4
LANES = 128

beta_first = 0.8
beta_second = 0.9
adam_eps = 1e-08
norm_eps = 1e-06
rate = 0.005

VMEM = pl.BlockSpec(memory_space=pltpu.VMEM)
SMEM = pl.BlockSpec(memory_space=pltpu.SMEM)
HBM = pl.BlockSpec(memory_space=pltpu.HBM)
FLAT = (((1,), (0,)), ((), ()))
TURNED = (((1,), (1,)), ((), ()))


def dot(a, b, dims):
    return lax.dot_general(a, b, dims, preferred_element_type=jnp.float32)


def in_hbm(value):
    return pltpu.with_memory_space_constraint(value, pltpu.HBM)


def in_vmem(value):
    return pltpu.with_memory_space_constraint(value, pltpu.VMEM)


def split_parts(values):
    high_part = values.astype(jnp.bfloat16)
    return high_part, (values - high_part.astype(jnp.float32)).astype(jnp.bfloat16)


def call(kernel, outs, specs, mib, scratch=()):
    return pl.pallas_call(
        kernel,
        out_shape=[
            out[2](out[0], out[1]) if len(out) == 3 else jax.ShapeDtypeStruct(*out) for out in outs
        ],
        in_specs=specs,
        out_specs=[HBM if pltpu.HBM in out else VMEM for out in outs],
        scratch_shapes=scratch,
        compiler_params=pltpu.CompilerParams(vmem_limit_bytes=mib * 1024 * 1024),
    )


def to_tiles(values, k, tiles, rest):
    ranks, spare = RANK // PARTS, values.shape[1] - LANES
    each = tiles.shape[0] // PARTS
    for p in range(PARTS):
        tiles[each * p + ranks * k : each * p + ranks * (k + 1), :] = values[ranks * p : ranks * (p + 1), :LANES]
    rest[:, :spare] = values[:, LANES:]
    row = [rest[pl.ds(r, PARTS, stride=ranks), :][:, :spare] for r in range(ranks)]
    tiles[pl.ds(2 * ranks + k, PARTS, stride=each), :] = jnp.concatenate(row, axis=1)


def from_tiles(tiles, k, values, rest):
    ranks, spare = RANK // PARTS, values.shape[1] - LANES
    each = tiles.shape[0] // PARTS
    for p in range(PARTS):
        values[ranks * p : ranks * (p + 1), :LANES] = tiles[each * p + ranks * k : each * p + ranks * (k + 1), :]
    row = tiles[pl.ds(2 * ranks + k, PARTS, stride=each), :]
    for r in range(ranks):
        rest[pl.ds(r, PARTS, stride=ranks), :] = jnp.concatenate([row[:, spare * r :], row[:, : spare * r]], axis=1) if r else row
    values[:, LANES:] = rest[:, :spare]


def pack_kernel(factor_out, factor_z, weight_out, weight_z, packed, weights, parts, both, sems):
    height = weight_out.shape[0]
    moves = [
        pltpu.make_async_copy(weight_out, both.at[pl.ds(0, height)], sems.at[2]),
        pltpu.make_async_copy(weight_z, both.at[pl.ds(height, height)], sems.at[3]),
        pltpu.make_async_copy(factor_out, parts.at[0], sems.at[0]),
        pltpu.make_async_copy(factor_z, parts.at[1], sems.at[1]),
    ]
    for move in moves:
        move.start()
    for move in moves[:2]:
        move.wait()
    out = pltpu.make_async_copy(both, weights, sems.at[2])
    out.start()
    for k in range(2):
        moves[2 + k].wait()
        packed[:, k * RANK : (k + 1) * RANK] = parts[k]
    out.wait()


def stage_kernel(source, kept, sems):
    height = source.shape[0] // CHUNKS
    moves = [
        pltpu.make_async_copy(
            source.at[pl.ds(height * c, height)], kept.at[pl.ds(height * c, height)], sems.at[c]
        )
        for c in range(CHUNKS)
    ]
    for move in moves:
        move.start()
    for move in moves:
        move.wait()


def gradient_kernel(
    cot, inp, own, other, gated, gate, partial, factor_out, factor_z, tokens, gates, projected, rest, sems, gate_sems
):
    moves = []
    for c in range(CHUNKS):
        height = tokens.shape[0] // CHUNKS
        at = pl.ds(height * c, height)
        moves.append(pltpu.make_async_copy(inp.at[at], tokens.at[at], sems.at[c]))
    gate_moves = [
        pltpu.make_async_copy(turned, gates.at[k], gate_sems.at[k]) for k, turned in enumerate((gated, gate))
    ]
    for move in (gate_moves[0], *moves, gate_moves[1]):
        move.start()

    rows = own.shape[0] // RINGS
    here = lax.axis_index("core") * rows
    there = rows - here
    for z in range(RINGS):
        for shard, place in ((own, here), (other, there)):
            block = shard[rows * z : rows * (z + 1), :]
            at = pl.ds(pl.multiple_of(2 * rows * z + place, 32), rows)
            factor_out[at, :] = block[:, :RANK]
            factor_z[at, :] = block[:, RANK:]

    for k, (side, factor) in enumerate(((cot, factor_out), (tokens, factor_z))):
        if k == 1:
            for move in moves:
                move.wait()
        for c in range(CHUNKS):
            at = pl.ds(height * c, height)
            projected[at, :] = dot(side[at, :], factor[...], FLAT)
        high, low = split_parts(projected[...])
        gate_moves[k].wait()
        total = dot(gates[k], high, FLAT) + dot(gates[k], low, FLAT)
        to_tiles(total.T, k, partial, rest)


def moments_kernel(arrived, first_out, second_out, first_z, second_z, *refs):
    *outs, tiles, part, side = refs
    ranks, width = first_out.shape
    spare = width - LANES
    each = arrived.shape[0] // PARTS
    total = arrived[:each, :]
    for p in range(1, PARTS):
        total = total + arrived[each * p : each * (p + 1), :]
    part[...] = total
    for k, (first, second) in enumerate(((first_out, second_out), (first_z, second_z))):
        last = 2 * ranks + k
        side[:, :LANES] = part[ranks * k : ranks * (k + 1), :]
        for r in range(ranks):
            side[r : r + 1, LANES:] = part[last : last + 1, spare * r : spare * (r + 1)]
        gradient = side[...]
        new_first = beta_first * first[...] + (1.0 - beta_first) * gradient
        new_second = beta_second * second[...] + (1.0 - beta_second) * gradient * gradient
        outs[2 * k][...] = new_first
        outs[2 * k + 1][...] = new_second
        ratio = new_first / (jnp.sqrt(new_second) + adam_eps)
        part[ranks * k : ranks * (k + 1), :] = ratio[:, :LANES]
        for r in range(ranks):
            part[last : last + 1, spare * r : spare * (r + 1)] = ratio[r : r + 1, LANES:]
    for p in range(PARTS):
        tiles[each * p : each * (p + 1), :] = part[...]


def ordered_kernel(weights, ordered, blocks, full, sems):
    columns = blocks.shape[2]
    half = PARTS // 2
    moves = [
        pltpu.make_async_copy(
            weights.at[pl.ds(half * k, half)], blocks.at[pl.ds(half * k, half)], sems.at[k]
        )
        for k in range(2)
    ]
    for move in moves:
        move.start()
    for k in range(PARTS):
        if k % half == 0:
            moves[k // half].wait()
        full[:, k * columns : (k + 1) * columns] = blocks[k]
    out = pltpu.make_async_copy(full, ordered, sems.at[0])
    out.start()
    out.wait()


def update_kernel(tiles, factor_out, factor_z, ordered, wide, narrow, full, sums, ratios, rest, sem):
    width, columns = narrow.shape[0] // 2, narrow.shape[1]
    move = pltpu.make_async_copy(ordered, full, sem)
    move.start()
    totals = []
    for k, factor in enumerate((factor_out, factor_z)):
        rows = pl.ds(k * width, width)
        from_tiles(tiles, k, ratios, rest)
        high, low = split_parts(ratios[...].T)
        update = dot(high, factor[...], TURNED) + dot(low, factor[...], TURNED)
        wide[rows, :] = update
        totals.append(jnp.sum(jnp.sum(update * update, axis=0, keepdims=True), axis=1, keepdims=True))
        mine = factor[pl.ds(pl.multiple_of(lax.axis_index(FS) * columns, 32), columns), :]
        narrow[rows, :] = dot(high, mine, TURNED) + dot(low, mine, TURNED)
    lane = lax.broadcasted_iota(jnp.int32, (1, 128), 1)
    row = jnp.where(lane < 64, totals[0], totals[1])
    sums[...] = jnp.broadcast_to(row[None], sums.shape)
    move.wait()


def final_kernel(sums, wide, narrow, full, copy_out, copy_z, step_out, step_z):
    width = step_out.shape[0]
    total = jnp.sum(sums[...], axis=0)
    scales = lax.rsqrt(total / (D * INNER) + norm_eps)
    for k, (copy, step) in enumerate(((copy_out, step_out), (copy_z, step_z))):
        scale = scales[:, 64 * k : 64 * k + 1]
        rows = pl.ds(k * width, width)
        step[...] = narrow[rows, :] * scale
        copy[...] = (full[rows, :] - rate * (wide[rows, :] * scale)).astype(jnp.bfloat16)


def per_device(
    block_in, out_cot, gated_out, gate_cot, factor_out, factor_z,
    weight_out, weight_z, first_out, second_out, first_z, second_z,
):
    f32, bf16 = jnp.float32, jnp.bfloat16
    width, columns = weight_out.shape
    ranks = first_z.shape[0]
    tokens = block_in.shape[0]

    rows_in_all = 2 * RANK * width // LANES

    def exchanged(tiles):
        shape = (PARTS, rows_in_all // PARTS // 2, 2, LANES)
        moved = lax.all_to_all(tiles.reshape(shape), FS, split_axis=0, concat_axis=0, tiled=True)
        return moved.reshape(tiles.shape)

    packed, weights = call(
        pack_kernel,
        [((columns, 2 * RANK), bf16), ((2 * width, columns), f32, pltpu.HBM)],
        [HBM] * 4,
        4,
        [
            pltpu.VMEM((2, columns, RANK), bf16),
            pltpu.VMEM((2 * width, columns), f32),
            pltpu.SemaphoreType.DMA((4,)),
        ],
    )(in_hbm(factor_out), in_hbm(factor_z), in_hbm(weight_out), in_hbm(weight_z.T))
    weights = lax.all_gather(weights, FS, axis=0, tiled=True).reshape(PARTS, 2 * width, columns)
    own = lax.all_gather(packed, "z", axis=0, tiled=True)
    other = lax.ppermute(own, "core", [(0, 1), (1, 0)])
    _, source = lax.optimization_barrier((own, out_cot))
    (staged,) = call(
        stage_kernel,
        [((tokens, D), bf16, pltpu.VMEM)],
        [HBM],
        2,
        [pltpu.SemaphoreType.DMA((CHUNKS,))],
    )(in_hbm(source))

    partial, full_out, full_z = call(
        gradient_kernel,
        [((rows_in_all, LANES), f32)] + [((D, RANK), bf16, pltpu.VMEM)] * 2,
        [VMEM, HBM, VMEM, VMEM, HBM, HBM],
        24,
        [
            pltpu.VMEM((tokens, D), bf16),
            pltpu.VMEM((2, width, tokens), bf16),
            pltpu.VMEM((tokens, RANK), f32),
            pltpu.VMEM((RANK, LANES), f32),
            pltpu.SemaphoreType.DMA((CHUNKS,)),
            pltpu.SemaphoreType.DMA((2,)),
        ],
    )(in_vmem(staged), in_hbm(block_in), in_vmem(own), in_vmem(other), in_hbm(gated_out.T), in_hbm(gate_cot.T))
    arrived = exchanged(partial)
    small = ((ranks, width), f32)
    *news, ratios = call(
        moments_kernel,
        [small] * 4 + [((rows_in_all, LANES), f32)],
        [VMEM] * 5,
        4,
        [pltpu.VMEM((rows_in_all // PARTS, LANES), f32), pltpu.VMEM((ranks, width), f32)],
    )(arrived, first_out.T, second_out.T, first_z, second_z)
    ratios = exchanged(ratios)
    (ordered,) = call(
        ordered_kernel,
        [((2 * width, D), f32, pltpu.HBM)],
        [HBM],
        16,
        [
            pltpu.VMEM((PARTS, 2 * width, columns), f32),
            pltpu.VMEM((2 * width, D), f32),
            pltpu.SemaphoreType.DMA((2,)),
        ],
    )(in_hbm(weights))
    wide, narrow, full, sums = call(
        update_kernel,
        [
            ((2 * width, D), f32, pltpu.VMEM),
            ((2 * width, columns), f32, pltpu.VMEM),
            ((2 * width, D), f32, pltpu.VMEM),
            ((TPS, 1, 128), f32),
        ],
        [VMEM, VMEM, VMEM, HBM],
        8,
        [pltpu.VMEM((RANK, width), f32), pltpu.VMEM((RANK, LANES), f32), pltpu.SemaphoreType.DMA],
    )(ratios, in_vmem(full_out), in_vmem(full_z), in_hbm(ordered))
    sums = lax.all_to_all(sums, TP, split_axis=0, concat_axis=0, tiled=True)
    copy_out, copy_z, step_out, step_z = call(
        final_kernel,
        [((width, D), bf16), ((width, D), bf16), ((width, columns), f32), ((width, columns), f32)],
        [VMEM] * 4,
        4,
    )(sums, in_vmem(wide), in_vmem(narrow), in_vmem(full))
    return (
        step_out, step_z.T, news[0].T, news[1].T, news[2], news[3], copy_out, copy_z.T,
    )


def solution(mesh):
    finer = Mesh(mesh.devices.reshape(RINGS, CORES, 8, 4), FS + TP)
    rows, both, turned = P(FS, None), P(FS, TP), P(TP, FS)
    return jax.shard_map(
        per_device,
        mesh=finer,
        in_specs=(
            rows, rows, both, both, rows, rows, turned, both, turned, turned, both, both,
        ),
        out_specs=(turned, both, turned, turned, both, both, P(TP, None), P(None, TP)),
        check_vma=False,
    )
```

```python
import jax
import jax.numpy as jnp
from jax import lax
from jax.experimental import pallas as pl
from jax.experimental.pallas import tpu as pltpu
from jax.sharding import Mesh
from jax.sharding import PartitionSpec as P

D = 2304
INNER = 4608
RANK = 192
FS = ("z", "core")
TP = ("y", "x")
RINGS, CORES = 12, 2
PARTS = RINGS * CORES
TPS = 32
CHUNKS = 4
BANDS = 3
LANES = 128

beta_first = 0.8
beta_second = 0.9
adam_eps = 1e-08
norm_eps = 1e-06
rate = 0.005

VMEM = pl.BlockSpec(memory_space=pltpu.VMEM)
SMEM = pl.BlockSpec(memory_space=pltpu.SMEM)
HBM = pl.BlockSpec(memory_space=pltpu.HBM)
FLAT = (((1,), (0,)), ((), ()))
TURNED = (((1,), (1,)), ((), ()))


def dot(a, b, dims):
    return lax.dot_general(a, b, dims, preferred_element_type=jnp.float32)


def in_hbm(value):
    return pltpu.with_memory_space_constraint(value, pltpu.HBM)


def in_vmem(value):
    return pltpu.with_memory_space_constraint(value, pltpu.VMEM)


def split_parts(values):
    high_part = values.astype(jnp.bfloat16)
    return high_part, (values - high_part.astype(jnp.float32)).astype(jnp.bfloat16)


def call(kernel, outs, specs, mib, scratch=()):
    return pl.pallas_call(
        kernel,
        out_shape=[
            out[2](out[0], out[1]) if len(out) == 3 else jax.ShapeDtypeStruct(*out) for out in outs
        ],
        in_specs=specs,
        out_specs=[HBM if pltpu.HBM in out else VMEM for out in outs],
        scratch_shapes=scratch,
        compiler_params=pltpu.CompilerParams(vmem_limit_bytes=mib * 1024 * 1024),
    )


def to_tiles(values, k, tiles, rest):
    ranks, spare = RANK // PARTS, values.shape[1] - LANES
    each = tiles.shape[0] // PARTS
    for p in range(PARTS):
        tiles[each * p + ranks * k : each * p + ranks * (k + 1), :] = values[ranks * p : ranks * (p + 1), :LANES]
    rest[:, :spare] = values[:, LANES:]
    row = [rest[pl.ds(r, PARTS, stride=ranks), :][:, :spare] for r in range(ranks)]
    tiles[pl.ds(2 * ranks + k, PARTS, stride=each), :] = jnp.concatenate(row, axis=1)


def from_tiles(tiles, k, values, rest):
    ranks, spare = RANK // PARTS, values.shape[1] - LANES
    each = tiles.shape[0] // PARTS
    for p in range(PARTS):
        values[ranks * p : ranks * (p + 1), :LANES] = tiles[each * p + ranks * k : each * p + ranks * (k + 1), :]
    row = tiles[pl.ds(2 * ranks + k, PARTS, stride=each), :]
    for r in range(ranks):
        rest[pl.ds(r, PARTS, stride=ranks), :] = jnp.concatenate([row[:, spare * r :], row[:, : spare * r]], axis=1) if r else row
    values[:, LANES:] = rest[:, :spare]


def pack_kernel(factor_out, factor_z, weight_out, weight_z, packed, weights, parts, both, dense, sems):
    height, columns = weight_out.shape
    moves = [
        pltpu.make_async_copy(weight_out, both.at[pl.ds(0, height)], sems.at[2]),
        pltpu.make_async_copy(weight_z, both.at[pl.ds(height, height)], sems.at[3]),
        pltpu.make_async_copy(factor_out, parts.at[0], sems.at[0]),
        pltpu.make_async_copy(factor_z, parts.at[1], sems.at[1]),
    ]
    for move in moves:
        move.start()
    for move in moves[:2]:
        move.wait()
    rows, spare = dense.shape[0], LANES - columns
    dense[:, :columns] = both[:rows, :]
    quarter = 2 * height - rows
    for j in range(rows // quarter):
        dense[quarter * j : quarter * (j + 1), columns:] = both[rows:, spare * j : spare * (j + 1)]
    out = pltpu.make_async_copy(dense, weights, sems.at[2])
    out.start()
    for k in range(2):
        moves[2 + k].wait()
        packed[:, k * RANK : (k + 1) * RANK] = parts[k]
    out.wait()


def stage_kernel(source, kept, sems):
    height = source.shape[0] // CHUNKS
    moves = [
        pltpu.make_async_copy(
            source.at[pl.ds(height * c, height)], kept.at[pl.ds(height * c, height)], sems.at[c]
        )
        for c in range(CHUNKS)
    ]
    for move in moves:
        move.start()
    for move in moves:
        move.wait()


def gradient_kernel(
    cot, inp, own, other, gated, gate, partial, factor_out, factor_z, tokens, gates, projected, rest, sems, gate_sems
):
    moves = []
    for c in range(CHUNKS):
        height = tokens.shape[0] // CHUNKS
        at = pl.ds(height * c, height)
        moves.append(pltpu.make_async_copy(inp.at[at], tokens.at[at], sems.at[c]))
    gate_moves = [
        pltpu.make_async_copy(turned, gates.at[k], gate_sems.at[k]) for k, turned in enumerate((gated, gate))
    ]
    for move in (gate_moves[0], *moves, gate_moves[1]):
        move.start()

    rows = own.shape[0] // RINGS
    here = lax.axis_index("core") * rows
    there = rows - here
    for z in range(RINGS):
        for shard, place in ((own, here), (other, there)):
            block = shard[rows * z : rows * (z + 1), :]
            at = pl.ds(pl.multiple_of(2 * rows * z + place, 32), rows)
            factor_out[at, :] = block[:, :RANK]
            factor_z[at, :] = block[:, RANK:]

    for k, (side, factor) in enumerate(((cot, factor_out), (tokens, factor_z))):
        if k == 1:
            for move in moves:
                move.wait()
        for c in range(CHUNKS):
            at = pl.ds(height * c, height)
            projected[at, :] = dot(side[at, :], factor[...], FLAT)
        high, low = split_parts(projected[...])
        gate_moves[k].wait()
        total = dot(gates[k], high, FLAT) + dot(gates[k], low, FLAT)
        to_tiles(total.T, k, partial, rest)


def moments_kernel(arrived, first_out, second_out, first_z, second_z, *refs):
    *outs, tiles, part, side = refs
    ranks, width = first_out.shape
    spare = width - LANES
    each = arrived.shape[0] // PARTS
    total = arrived[:each, :]
    for p in range(1, PARTS):
        total = total + arrived[each * p : each * (p + 1), :]
    part[...] = total
    for k, (first, second) in enumerate(((first_out, second_out), (first_z, second_z))):
        last = 2 * ranks + k
        side[:, :LANES] = part[ranks * k : ranks * (k + 1), :]
        for r in range(ranks):
            side[r : r + 1, LANES:] = part[last : last + 1, spare * r : spare * (r + 1)]
        gradient = side[...]
        new_first = beta_first * first[...] + (1.0 - beta_first) * gradient
        new_second = beta_second * second[...] + (1.0 - beta_second) * gradient * gradient
        outs[2 * k][...] = new_first
        outs[2 * k + 1][...] = new_second
        ratio = new_first / (jnp.sqrt(new_second) + adam_eps)
        part[ranks * k : ranks * (k + 1), :] = ratio[:, :LANES]
        for r in range(ranks):
            part[last : last + 1, spare * r : spare * (r + 1)] = ratio[r : r + 1, LANES:]
    for p in range(PARTS):
        tiles[each * p : each * (p + 1), :] = part[...]


def ordered_kernel(weights, ordered, blocks, full, sems):
    rows, columns = blocks.shape[1], full.shape[1] // PARTS
    quarter, spare = full.shape[0] - rows, LANES - columns
    half = PARTS // 2
    moves = [
        pltpu.make_async_copy(
            weights.at[pl.ds(half * k, half)], blocks.at[pl.ds(half * k, half)], sems.at[k]
        )
        for k in range(2)
    ]
    for move in moves:
        move.start()
    for k in range(PARTS):
        if k % half == 0:
            moves[k // half].wait()
        at = k * columns
        full[:rows, at : at + columns] = blocks[k, :, :columns]
        for j in range(rows // quarter):
            full[rows:, at + spare * j : at + spare * (j + 1)] = blocks[
                k, quarter * j : quarter * (j + 1), columns:
            ]
    out = pltpu.make_async_copy(full, ordered, sems.at[0])
    out.start()
    out.wait()


def update_kernel(tiles, factor_out, factor_z, ordered, wide, narrow, full, sums, ratios, rest, sem):
    width, columns = narrow.shape[0] // 2, narrow.shape[1]
    move = pltpu.make_async_copy(ordered, full, sem)
    move.start()
    totals = []
    for k, factor in enumerate((factor_out, factor_z)):
        rows = pl.ds(k * width, width)
        from_tiles(tiles, k, ratios, rest)
        both = jnp.concatenate(split_parts(ratios[...].T), axis=0)
        squares = jnp.zeros((1, 2 * LANES), jnp.float32)
        for n in range(0, D, 2 * LANES):
            terms = dot(both, factor[n : n + 2 * LANES, :], TURNED)
            update = terms[:width] + terms[width:]
            wide[rows, n : n + 2 * LANES] = update
            squares = squares + jnp.sum(update * update, axis=0, keepdims=True)
        totals.append(jnp.sum(squares, axis=1, keepdims=True))
        mine = factor[pl.ds(pl.multiple_of(lax.axis_index(FS) * columns, 32), columns), :]
        terms = dot(both, mine, TURNED)
        narrow[rows, :] = terms[:width] + terms[width:]
    lane = lax.broadcasted_iota(jnp.int32, (1, LANES), 1)
    row = jnp.where(lane < LANES // 2, totals[0], totals[1])
    sums[...] = jnp.broadcast_to(row[None], sums.shape)
    move.wait()


def final_kernel(
    sums, wide, narrow, full, copy_out, copy_z, step_out, step_z, copies, steps, copy_sems, step_sems
):
    width = step_out.shape[0]
    height = width // BANDS
    total = jnp.sum(sums[...], axis=0)
    scales = lax.rsqrt(total / (D * INNER) + norm_eps)
    moves = []
    for k, (copy, step) in enumerate(((copy_out, step_out), (copy_z, step_z))):
        scale = scales[:, LANES // 2 * k : LANES // 2 * k + 1]
        for c in range(BANDS):
            rows = pl.ds(k * width + height * c, height)
            copies[rows, :] = (full[rows, :] - rate * (wide[rows, :] * scale)).astype(jnp.bfloat16)
            moves.append(
                pltpu.make_async_copy(copies.at[rows], copy.at[pl.ds(height * c, height)], copy_sems.at[k, c])
            )
            moves[-1].start()
        rows = pl.ds(k * width, width)
        steps[rows, :] = narrow[rows, :] * scale
        moves.append(pltpu.make_async_copy(steps.at[rows], step, step_sems.at[k]))
        moves[-1].start()
    for move in moves:
        move.wait()


def per_device(
    block_in, out_cot, gated_out, gate_cot, factor_out, factor_z,
    weight_out, weight_z, first_out, second_out, first_z, second_z,
):
    f32, bf16 = jnp.float32, jnp.bfloat16
    width, columns = weight_out.shape
    ranks = first_z.shape[0]
    tokens = block_in.shape[0]

    rows_in_all = 2 * RANK * width // LANES
    dense = 2 * width * columns // LANES

    def exchanged(tiles):
        shape = (PARTS, rows_in_all // PARTS // 2, 2, LANES)
        moved = lax.all_to_all(tiles.reshape(shape), FS, split_axis=0, concat_axis=0, tiled=True)
        return moved.reshape(tiles.shape)

    packed, weights = call(
        pack_kernel,
        [((columns, 2 * RANK), bf16), ((dense, LANES), f32, pltpu.HBM)],
        [HBM] * 4,
        4,
        [
            pltpu.VMEM((2, columns, RANK), bf16),
            pltpu.VMEM((2 * width, columns), f32),
            pltpu.VMEM((dense, LANES), f32),
            pltpu.SemaphoreType.DMA((4,)),
        ],
    )(in_hbm(factor_out), in_hbm(factor_z), in_hbm(weight_out), in_hbm(weight_z.T))
    weights = lax.all_gather(weights, FS, axis=0, tiled=True).reshape(PARTS, dense, LANES)
    own = lax.all_gather(packed, "z", axis=0, tiled=True)
    other = lax.ppermute(own, "core", [(0, 1), (1, 0)])
    _, source = lax.optimization_barrier((own, out_cot))
    (staged,) = call(
        stage_kernel,
        [((tokens, D), bf16, pltpu.VMEM)],
        [HBM],
        2,
        [pltpu.SemaphoreType.DMA((CHUNKS,))],
    )(in_hbm(source))

    partial, full_out, full_z = call(
        gradient_kernel,
        [((rows_in_all, LANES), f32)] + [((D, RANK), bf16, pltpu.VMEM)] * 2,
        [VMEM, HBM, VMEM, VMEM, HBM, HBM],
        24,
        [
            pltpu.VMEM((tokens, D), bf16),
            pltpu.VMEM((2, width, tokens), bf16),
            pltpu.VMEM((tokens, RANK), f32),
            pltpu.VMEM((RANK, LANES), f32),
            pltpu.SemaphoreType.DMA((CHUNKS,)),
            pltpu.SemaphoreType.DMA((2,)),
        ],
    )(in_vmem(staged), in_hbm(block_in), in_vmem(own), in_vmem(other), in_hbm(gated_out.T), in_hbm(gate_cot.T))
    arrived = exchanged(partial)
    small = ((ranks, width), f32)
    *news, ratios = call(
        moments_kernel,
        [small] * 4 + [((rows_in_all, LANES), f32)],
        [VMEM] * 5,
        4,
        [pltpu.VMEM((rows_in_all // PARTS, LANES), f32), pltpu.VMEM((ranks, width), f32)],
    )(arrived, first_out.T, second_out.T, first_z, second_z)
    ratios = exchanged(ratios)
    (ordered,) = call(
        ordered_kernel,
        [((2 * width, D), f32, pltpu.HBM)],
        [HBM],
        16,
        [
            pltpu.VMEM((PARTS, dense, LANES), f32),
            pltpu.VMEM((2 * width, D), f32),
            pltpu.SemaphoreType.DMA((2,)),
        ],
    )(in_hbm(weights))
    wide, narrow, full, sums = call(
        update_kernel,
        [
            ((2 * width, D), f32, pltpu.VMEM),
            ((2 * width, columns), f32, pltpu.VMEM),
            ((2 * width, D), f32, pltpu.VMEM),
            ((TPS, 1, 128), f32),
        ],
        [VMEM, VMEM, VMEM, HBM],
        8,
        [pltpu.VMEM((RANK, width), f32), pltpu.VMEM((RANK, LANES), f32), pltpu.SemaphoreType.DMA],
    )(ratios, in_vmem(full_out), in_vmem(full_z), in_hbm(ordered))
    sums = lax.all_to_all(sums, TP, split_axis=0, concat_axis=0, tiled=True)
    copy_out, copy_z, step_out, step_z = call(
        final_kernel,
        [((width, D), bf16, pltpu.HBM)] * 2 + [((width, columns), f32, pltpu.HBM)] * 2,
        [VMEM] * 4,
        4,
        [
            pltpu.VMEM((2 * width, D), bf16),
            pltpu.VMEM((2 * width, columns), f32),
            pltpu.SemaphoreType.DMA((2, BANDS)),
            pltpu.SemaphoreType.DMA((2,)),
        ],
    )(sums, in_vmem(wide), in_vmem(narrow), in_vmem(full))
    return (
        step_out, step_z.T, news[0].T, news[1].T, news[2], news[3], copy_out, copy_z.T,
    )


def solution(mesh):
    finer = Mesh(mesh.devices.reshape(RINGS, CORES, 8, 4), FS + TP)
    rows, both, turned = P(FS, None), P(FS, TP), P(TP, FS)
    return jax.shard_map(
        per_device,
        mesh=finer,
        in_specs=(
            rows, rows, both, both, rows, rows, turned, both, turned, turned, both, both,
        ),
        out_specs=(turned, both, turned, turned, both, both, P(TP, None), P(None, TP)),
        check_vma=False,
    )
```

```python
import jax
import jax.numpy as jnp
from jax import lax
from jax.experimental import pallas as pl
from jax.experimental.pallas import tpu as pltpu
from jax.sharding import Mesh
from jax.sharding import PartitionSpec as P


D = 2304
INNER = 4608
RANK = 192
FS = ("z", "core")
TP = ("y", "x")
RINGS, CORES = 12, 2
PARTS = RINGS * CORES
TPS = 32
CHUNKS = 4
BANDS = 3
LANES = 128

beta_first = 0.8
beta_second = 0.9
adam_eps = 1e-08
norm_eps = 1e-06
rate = 0.005

VMEM = pl.BlockSpec(memory_space=pltpu.VMEM)
SMEM = pl.BlockSpec(memory_space=pltpu.SMEM)
HBM = pl.BlockSpec(memory_space=pltpu.HBM)
FLAT = (((1,), (0,)), ((), ()))
TURNED = (((1,), (1,)), ((), ()))


def dot(a, b, dims):
    return lax.dot_general(a, b, dims, preferred_element_type=jnp.float32)


def in_hbm(value):
    return pltpu.with_memory_space_constraint(value, pltpu.HBM)


def in_vmem(value):
    return pltpu.with_memory_space_constraint(value, pltpu.VMEM)


def split_parts(values):
    high_part = values.astype(jnp.bfloat16)
    return high_part, (values - high_part.astype(jnp.float32)).astype(jnp.bfloat16)


def call(kernel, outs, specs, mib, scratch=()):
    return pl.pallas_call(
        kernel,
        out_shape=[
            out[2](out[0], out[1]) if len(out) == 3 else jax.ShapeDtypeStruct(*out) for out in outs
        ],
        in_specs=specs,
        out_specs=[HBM if pltpu.HBM in out else VMEM for out in outs],
        scratch_shapes=scratch,
        compiler_params=pltpu.CompilerParams(vmem_limit_bytes=mib * 1024 * 1024),
    )


def to_tiles(values, k, tiles, rest):
    ranks, spare = RANK // PARTS, values.shape[1] - LANES
    each = tiles.shape[0] // PARTS
    for p in range(PARTS):
        tiles[each * p + ranks * k : each * p + ranks * (k + 1), :] = values[ranks * p : ranks * (p + 1), :LANES]
    rest[:, :spare] = values[:, LANES:]
    row = [rest[pl.ds(r, PARTS, stride=ranks), :][:, :spare] for r in range(ranks)]
    tiles[pl.ds(2 * ranks + k, PARTS, stride=each), :] = jnp.concatenate(row, axis=1)


def from_tiles(tiles, k, values, rest):
    ranks, spare = RANK // PARTS, values.shape[1] - LANES
    each = tiles.shape[0] // PARTS
    for p in range(PARTS):
        values[ranks * p : ranks * (p + 1), :LANES] = tiles[each * p + ranks * k : each * p + ranks * (k + 1), :]
    row = tiles[pl.ds(2 * ranks + k, PARTS, stride=each), :]
    for r in range(ranks):
        rest[pl.ds(r, PARTS, stride=ranks), :] = jnp.concatenate([row[:, spare * r :], row[:, : spare * r]], axis=1) if r else row
    values[:, LANES:] = rest[:, :spare]


def pack_kernel(factor_out, factor_z, weight_out, weight_z, packed, weights, parts, both, dense, sems):
    height, columns = weight_out.shape
    moves = [
        pltpu.make_async_copy(weight_out, both.at[pl.ds(0, height)], sems.at[2]),
        pltpu.make_async_copy(weight_z, both.at[pl.ds(height, height)], sems.at[3]),
        pltpu.make_async_copy(factor_out, parts.at[0], sems.at[0]),
        pltpu.make_async_copy(factor_z, parts.at[1], sems.at[1]),
    ]
    for move in moves:
        move.start()
    for move in moves[:2]:
        move.wait()
    rows, spare = dense.shape[0], LANES - columns
    dense[:, :columns] = both[:rows, :]
    quarter = 2 * height - rows
    for j in range(rows // quarter):
        dense[quarter * j : quarter * (j + 1), columns:] = both[rows:, spare * j : spare * (j + 1)]
    out = pltpu.make_async_copy(dense, weights, sems.at[2])
    out.start()
    for k in range(2):
        moves[2 + k].wait()
        packed[:, k * RANK : (k + 1) * RANK] = parts[k]
    out.wait()


def stage_kernel(source, kept, sems):
    height = source.shape[0] // CHUNKS
    moves = [
        pltpu.make_async_copy(
            source.at[pl.ds(height * c, height)], kept.at[pl.ds(height * c, height)], sems.at[c]
        )
        for c in range(CHUNKS)
    ]
    for move in moves:
        move.start()
    for move in moves:
        move.wait()


def gradient_kernel(
    cot, inp, own, other, gated, gate, partial, factor_out, factor_z, tokens, gates, projected, rest, sems, gate_sems
):
    moves = []
    for c in range(CHUNKS):
        height = tokens.shape[0] // CHUNKS
        at = pl.ds(height * c, height)
        moves.append(pltpu.make_async_copy(inp.at[at], tokens.at[at], sems.at[c]))
    gate_moves = [
        pltpu.make_async_copy(turned, gates.at[k], gate_sems.at[k]) for k, turned in enumerate((gated, gate))
    ]
    for move in (gate_moves[0], *moves, gate_moves[1]):
        move.start()

    rows = own.shape[0] // RINGS
    here = lax.axis_index("core") * rows
    there = rows - here
    for z in range(RINGS):
        for shard, place in ((own, here), (other, there)):
            block = shard[rows * z : rows * (z + 1), :]
            at = pl.ds(pl.multiple_of(2 * rows * z + place, 32), rows)
            factor_out[at, :] = block[:, :RANK]
            factor_z[at, :] = block[:, RANK:]

    for k, (side, factor) in enumerate(((cot, factor_out), (tokens, factor_z))):
        if k == 1:
            for move in moves:
                move.wait()
        for c in range(CHUNKS):
            at = pl.ds(height * c, height)
            projected[at, :] = dot(side[at, :], factor[...], FLAT)
        high, low = split_parts(projected[...])
        gate_moves[k].wait()
        total = dot(gates[k], high, FLAT) + dot(gates[k], low, FLAT)
        to_tiles(total.T, k, partial, rest)


def moments_kernel(arrived, first_out, second_out, first_z, second_z, *refs):
    *outs, tiles, part, side = refs
    ranks, width = first_out.shape
    spare = width - LANES
    each = arrived.shape[0] // PARTS
    total = arrived[:each, :]
    for p in range(1, PARTS):
        total = total + arrived[each * p : each * (p + 1), :]
    part[...] = total
    for k, (first, second) in enumerate(((first_out, second_out), (first_z, second_z))):
        last = 2 * ranks + k
        side[:, :LANES] = part[ranks * k : ranks * (k + 1), :]
        for r in range(ranks):
            side[r : r + 1, LANES:] = part[last : last + 1, spare * r : spare * (r + 1)]
        gradient = side[...]
        new_first = beta_first * first[...] + (1.0 - beta_first) * gradient
        new_second = beta_second * second[...] + (1.0 - beta_second) * gradient * gradient
        outs[2 * k][...] = new_first
        outs[2 * k + 1][...] = new_second
        ratio = new_first / (jnp.sqrt(new_second) + adam_eps)
        part[ranks * k : ranks * (k + 1), :] = ratio[:, :LANES]
        for r in range(ranks):
            part[last : last + 1, spare * r : spare * (r + 1)] = ratio[r : r + 1, LANES:]
    for p in range(PARTS):
        tiles[each * p : each * (p + 1), :] = part[...]


def gate_kernel(value, source, kept):
    del value, source, kept


def ordered_kernel(own, other, ordered, blocks, full, sems):
    rows, columns = blocks.shape[2], full.shape[1] // PARTS
    quarter, spare = full.shape[0] - rows, LANES - columns
    here = lax.axis_index("core")
    moves = [
        pltpu.make_async_copy(own, blocks.at[:, here], sems.at[0]),
        pltpu.make_async_copy(other, blocks.at[:, 1 - here], sems.at[1]),
    ]
    for move in moves:
        move.start()
    for move in moves:
        move.wait()
    for k in range(PARTS):
        at, block = k * columns, blocks.at[k // CORES, k % CORES]
        full[:rows, at : at + columns] = block[:, :columns]
        for j in range(rows // quarter):
            full[rows:, at + spare * j : at + spare * (j + 1)] = block[
                quarter * j : quarter * (j + 1), columns:
            ]
    out = pltpu.make_async_copy(full, ordered, sems.at[0])
    out.start()
    out.wait()


def update_kernel(tiles, factor_out, factor_z, ordered, wide, narrow, full, sums, ratios, rest, sem):
    width, columns = narrow.shape[0] // 2, narrow.shape[1]
    move = pltpu.make_async_copy(ordered, full, sem)
    move.start()
    totals = []
    for k, factor in enumerate((factor_out, factor_z)):
        rows = pl.ds(k * width, width)
        from_tiles(tiles, k, ratios, rest)
        both = jnp.concatenate(split_parts(ratios[...].T), axis=0)
        squares = jnp.zeros((1, 2 * LANES), jnp.float32)
        for n in range(0, D, 2 * LANES):
            terms = dot(both, factor[n : n + 2 * LANES, :], TURNED)
            update = terms[:width] + terms[width:]
            wide[rows, n : n + 2 * LANES] = update
            squares = squares + jnp.sum(update * update, axis=0, keepdims=True)
        totals.append(jnp.sum(squares, axis=1, keepdims=True))
        mine = factor[pl.ds(pl.multiple_of(lax.axis_index(FS) * columns, 32), columns), :]
        terms = dot(both, mine, TURNED)
        narrow[rows, :] = terms[:width] + terms[width:]
    lane = lax.broadcasted_iota(jnp.int32, (1, LANES), 1)
    row = jnp.where(lane < LANES // 2, totals[0], totals[1])
    sums[...] = jnp.broadcast_to(row[None], sums.shape)
    move.wait()


def final_kernel(
    sums, wide, narrow, full, copy_out, copy_z, step_out, step_z, copies, steps, copy_sems, step_sems
):
    width = step_out.shape[0]
    height = width // BANDS
    total = jnp.sum(sums[...], axis=0)
    scales = lax.rsqrt(total / (D * INNER) + norm_eps)
    moves = []
    for k, (copy, step) in enumerate(((copy_out, step_out), (copy_z, step_z))):
        scale = scales[:, LANES // 2 * k : LANES // 2 * k + 1]
        for c in range(BANDS):
            rows = pl.ds(k * width + height * c, height)
            copies[rows, :] = (full[rows, :] - rate * (wide[rows, :] * scale)).astype(jnp.bfloat16)
            moves.append(
                pltpu.make_async_copy(copies.at[rows], copy.at[pl.ds(height * c, height)], copy_sems.at[k, c])
            )
            moves[-1].start()
        rows = pl.ds(k * width, width)
        steps[rows, :] = narrow[rows, :] * scale
        moves.append(pltpu.make_async_copy(steps.at[rows], step, step_sems.at[k]))
        moves[-1].start()
    for move in moves:
        move.wait()


def per_device(
    block_in, out_cot, gated_out, gate_cot, factor_out, factor_z,
    weight_out, weight_z, first_out, second_out, first_z, second_z,
):
    f32, bf16 = jnp.float32, jnp.bfloat16
    width, columns = weight_out.shape
    ranks = first_z.shape[0]
    tokens = block_in.shape[0]

    rows_in_all = 2 * RANK * width // LANES
    dense = 2 * width * columns // LANES

    def exchanged(tiles):
        shape = (PARTS, rows_in_all // PARTS // 2, 2, LANES)
        moved = lax.all_to_all(tiles.reshape(shape), FS, split_axis=0, concat_axis=0, tiled=True)
        return moved.reshape(tiles.shape)

    packed, weights = call(
        pack_kernel,
        [((columns, 2 * RANK), bf16), ((dense, LANES), f32, pltpu.HBM)],
        [HBM] * 4,
        4,
        [
            pltpu.VMEM((2, columns, RANK), bf16),
            pltpu.VMEM((2 * width, columns), f32),
            pltpu.VMEM((dense, LANES), f32),
            pltpu.SemaphoreType.DMA((4,)),
        ],
    )(in_hbm(factor_out), in_hbm(factor_z), in_hbm(weight_out), in_hbm(weight_z.T))
    weights = lax.all_gather(weights, "z", axis=0, tiled=True)
    own = lax.all_gather(packed, "z", axis=0, tiled=True)
    other = lax.ppermute(own, "core", [(0, 1), (1, 0)])
    _, source = lax.optimization_barrier((own, out_cot))
    (staged,) = call(
        stage_kernel,
        [((tokens, D), bf16, pltpu.VMEM)],
        [HBM],
        2,
        [pltpu.SemaphoreType.DMA((CHUNKS,))],
    )(in_hbm(source))

    partial, full_out, full_z = call(
        gradient_kernel,
        [((rows_in_all, LANES), f32)] + [((D, RANK), bf16, pltpu.VMEM)] * 2,
        [VMEM, HBM, VMEM, VMEM, HBM, HBM],
        24,
        [
            pltpu.VMEM((tokens, D), bf16),
            pltpu.VMEM((2, width, tokens), bf16),
            pltpu.VMEM((tokens, RANK), f32),
            pltpu.VMEM((RANK, LANES), f32),
            pltpu.SemaphoreType.DMA((CHUNKS,)),
            pltpu.SemaphoreType.DMA((2,)),
        ],
    )(in_vmem(staged), in_hbm(block_in), in_vmem(own), in_vmem(other), in_hbm(gated_out.T), in_hbm(gate_cot.T))
    arrived = exchanged(partial)
    small = ((ranks, width), f32)
    *news, ratios = call(
        moments_kernel,
        [small] * 4 + [((rows_in_all, LANES), f32)],
        [VMEM] * 5,
        4,
        [pltpu.VMEM((rows_in_all // PARTS, LANES), f32), pltpu.VMEM((ranks, width), f32)],
    )(arrived, first_out.T, second_out.T, first_z, second_z)
    weights = pl.pallas_call(
        gate_kernel,
        out_shape=pltpu.HBM(weights.shape, f32),
        in_specs=[HBM, HBM],
        out_specs=HBM,
        input_output_aliases={1: 0},
    )(in_hbm(news[2]), in_hbm(weights))
    ratios = exchanged(ratios)
    others = lax.ppermute(weights, "core", [(0, 1), (1, 0)])
    blocks = (RINGS, dense, LANES)
    (ordered,) = call(
        ordered_kernel,
        [((2 * width, D), f32, pltpu.HBM)],
        [HBM] * 2,
        16,
        [
            pltpu.VMEM((RINGS, CORES, dense, LANES), f32),
            pltpu.VMEM((2 * width, D), f32),
            pltpu.SemaphoreType.DMA((2,)),
        ],
    )(in_hbm(weights.reshape(blocks)), in_hbm(others.reshape(blocks)))
    wide, narrow, full, sums = call(
        update_kernel,
        [
            ((2 * width, D), f32, pltpu.VMEM),
            ((2 * width, columns), f32, pltpu.VMEM),
            ((2 * width, D), f32, pltpu.VMEM),
            ((TPS, 1, 128), f32),
        ],
        [VMEM, VMEM, VMEM, HBM],
        8,
        [pltpu.VMEM((RANK, width), f32), pltpu.VMEM((RANK, LANES), f32), pltpu.SemaphoreType.DMA],
    )(ratios, in_vmem(full_out), in_vmem(full_z), in_hbm(ordered))
    sums = lax.all_to_all(sums, TP, split_axis=0, concat_axis=0, tiled=True)
    copy_out, copy_z, step_out, step_z = call(
        final_kernel,
        [((width, D), bf16, pltpu.HBM)] * 2 + [((width, columns), f32, pltpu.HBM)] * 2,
        [VMEM] * 4,
        4,
        [
            pltpu.VMEM((2 * width, D), bf16),
            pltpu.VMEM((2 * width, columns), f32),
            pltpu.SemaphoreType.DMA((2, BANDS)),
            pltpu.SemaphoreType.DMA((2,)),
        ],
    )(sums, in_vmem(wide), in_vmem(narrow), in_vmem(full))
    return (
        step_out, step_z.T, news[0].T, news[1].T, news[2], news[3], copy_out, copy_z.T,
    )


def solution(mesh):
    finer = Mesh(mesh.devices.reshape(RINGS, CORES, 8, 4), FS + TP)
    rows, both, turned = P(FS, None), P(FS, TP), P(TP, FS)
    return jax.shard_map(
        per_device,
        mesh=finer,
        in_specs=(
            rows, rows, both, both, rows, rows, turned, both, turned, turned, both, both,
        ),
        out_specs=(turned, both, turned, turned, both, both, P(TP, None), P(None, TP)),
        check_vma=False,
    )
```
